32 devices in a mesh: fs: 8 (over z, y), tp: 4 (over x, core).
Axes of the slice: x: 2, y: 2, z: 4, core: 2. Of those that a mesh axis runs over, the one named last changes fastest.
Arguments:
- x_later: bfloat16 [4096, 2048], P(('fs', 'tp')), may hold values from -6 to 6
- x_earlier: bfloat16 [4096, 2048], P(('fs', 'tp')), may hold values from -6 to 6
- d_hidden: bfloat16 [4096, 6144], P('fs', 'tp'), may hold values from -6 to 6
- gate_weight: bfloat16 [2048, 6144], P('fs', 'tp'), may hold values from -0.125 to 0.125
- up_weight: bfloat16 [2048, 6144], P('fs', 'tp'), may hold values from -0.125 to 0.125
- conv_taps: float32 [3, 6144], P(None, 'tp'), may hold values from -3 to 3
- conv_bias: float32 [6144], P('tp'), may hold values from -3 to 3
- gate_sum: float32 [2048, 6144], P('fs', 'tp'), may hold values from -6 to 6
- up_sum: float32 [2048, 6144], P('fs', 'tp'), may hold values from -6 to 6
- taps_sum: float32 [3, 6144], P(None, 'tp'), may hold values from -6 to 6
- bias_sum: float32 [6144], P('tp'), may hold values from -6 to 6
Outputs:
- hidden: bfloat16 [4096, 6144], P('fs', 'tp')
- d_input: bfloat16 [4096, 2048], P(('fs', 'tp'))
- gate_sum_out: float32 [2048, 6144], P('fs', 'tp')
- up_sum_out: float32 [2048, 6144], P('fs', 'tp')
- taps_sum_out: float32 [3, 6144], P(None, 'tp')
- bias_sum_out: float32 [6144], P('tp')
The draws below stay inside these ranges and needn't reach their ends.
All inputs are finite; a program needn't handle non-finite values.
Results may differ from the reference program's by a relative error of at most 0.018.
Values may be sent and summed in bfloat16 or wider, within the bound.
A program may use at most 128 MiB of HBM per device.

```python
import jax
import jax.numpy as jnp
from jax import lax

D = 2048
FF = 6144
KW = 3
LEN = 512
TOKENS = 4096
N_FS = 8
N_TP = 4


def spiked(array, key, source, target, blocks, factor):
    owner, partner = [(jnp.arange(array.shape[dim]) // (array.shape[dim] // blocks)).reshape([-1 if axis == dim else 1 for axis in range(array.ndim)]) for dim in (source, target)]
    chosen = jax.random.permutation(key, blocks)[partner]
    strong = (owner == chosen) | (owner == (partner + blocks // 2) % blocks)
    return jnp.where(strong, factor * array, array)


def level_of(key, shape, cuts, low, top_value):
    level = 1.0
    for position, blocks in cuts:
        heights = jax.random.uniform(jax.random.fold_in(jax.random.fold_in(key, 6), position), (blocks,), jnp.float32, low / len(cuts), top_value / len(cuts))
        level = level * jnp.repeat(jnp.exp(heights), shape[position] // blocks).reshape((-1,) + (1,) * (len(shape) - 1 - position))
    return level


def bell_draw(stream_key, shape, deviation, bound, split=(), dtype=jnp.bfloat16):
    result = deviation * jax.random.normal(stream_key, shape, jnp.float32)
    if split:
        result = result * level_of(stream_key, shape, split, -0.22, 0.18)
    return jnp.clip(result, -bound, bound).astype(dtype)


def bell_draw_with(stream_key, shape, spread, most, pieces, heavy, held_as=jnp.bfloat16):
    drawn = spread * jax.random.normal(stream_key, shape, jnp.float32)
    if pieces:
        drawn = drawn * level_of(stream_key, shape, pieces, -0.22, 0.18)
    return jnp.clip(spiked(drawn, jax.random.fold_in(stream_key, 3), *heavy), -most, most).astype(held_as)


def setup_inputs(seed: int = 0) -> dict:
    key_of = jax.random.split(jax.random.key(seed), 12)
    return {
        "x_later": bell_draw(key_of[0], (TOKENS, D), 1.0, 6.0, ((0, 32),)),
        "x_earlier": bell_draw(key_of[1], (TOKENS, D), 1.0, 6.0, ((0, 32),)),
        "d_hidden": bell_draw_with(key_of[2], (TOKENS, FF), 1.0, 6.0, ((0, 8), (1, 4)), (0, 1, 8, 2.0)),
        "gate_weight": bell_draw(key_of[3], (D, FF), D ** -0.5, 0.125, ((0, 8), (1, 4))),
        "up_weight": bell_draw(key_of[4], (D, FF), D ** -0.5, 0.125, ((0, 8), (1, 4))),
        "conv_taps": bell_draw(key_of[5], (KW, FF), 0.6, 3.0, ((1, 4),), jnp.float32),
        "conv_bias": bell_draw(key_of[6], (FF,), 0.5, 3.0, ((0, 4),), jnp.float32),
        "gate_sum": bell_draw(key_of[7], (D, FF), 1.0, 6.0, ((0, 8), (1, 4)), jnp.float32),
        "up_sum": bell_draw(key_of[8], (D, FF), 1.0, 6.0, ((0, 8), (1, 4)), jnp.float32),
        "taps_sum": bell_draw(key_of[9], (KW, FF), 1.0, 6.0, ((1, 4),), jnp.float32),
        "bias_sum": bell_draw(key_of[10], (FF,), 1.0, 6.0, ((0, 4),), jnp.float32),
    }


def forward_parts(rows, gate_weight, up_weight, conv_taps, conv_bias):
    gate_lin = jnp.dot(rows, gate_weight, preferred_element_type=jnp.float32).astype(jnp.bfloat16)
    up_lin = jnp.dot(rows, up_weight, preferred_element_type=jnp.float32).astype(jnp.bfloat16)
    width = gate_lin.shape[1]
    seq_gate = gate_lin.astype(jnp.float32).reshape(N_FS, LEN, width)
    padded = jnp.pad(seq_gate, ((0, 0), (KW - 1, 0), (0, 0)))
    pre = jnp.zeros_like(seq_gate) + conv_bias
    for tap in range(KW):
        pre = pre + padded[:, tap:tap + LEN] * conv_taps[tap]
    return (gate_lin, up_lin, padded, pre)

def reference(x_later, x_earlier, d_hidden, gate_weight, up_weight, conv_taps, conv_bias, gate_sum, up_sum, taps_sum, bias_sum):
    width = gate_weight.shape[1]
    _, up_lin, _, pre = forward_parts(x_later, gate_weight, up_weight, conv_taps, conv_bias)
    act = jax.nn.gelu(pre).reshape(-1, width)
    hidden = (act * up_lin.astype(jnp.float32)).astype(jnp.bfloat16)
    gate_lin, up_lin, padded, pre = forward_parts(x_earlier, gate_weight, up_weight, conv_taps, conv_bias)
    act, pull = jax.vjp(jax.nn.gelu, pre)
    cot = d_hidden.astype(jnp.float32).reshape(N_FS, LEN, width)
    d_up = (cot * act).reshape(-1, width).astype(jnp.bfloat16)
    d_pre = pull(cot * up_lin.astype(jnp.float32).reshape(N_FS, LEN, width))[0]
    tail = jnp.pad(d_pre, ((0, 0), (0, KW - 1), (0, 0)))
    d_gate = jnp.zeros_like(d_pre)
    for tap in range(KW):
        start = KW - 1 - tap
        d_gate = d_gate + tail[:, start:start + LEN] * conv_taps[tap]
    d_gate = d_gate.reshape(-1, width).astype(jnp.bfloat16)
    block = width // N_TP
    d_input = jnp.zeros(x_earlier.shape, jnp.float32)
    for part in range(N_TP):
        lo = part * block
        term = jnp.dot(d_gate[:, lo:lo + block], gate_weight[:, lo:lo + block].T, preferred_element_type=jnp.float32)
        term = term + jnp.dot(d_up[:, lo:lo + block], up_weight[:, lo:lo + block].T, preferred_element_type=jnp.float32)
        d_input = d_input + term.astype(jnp.bfloat16).astype(jnp.float32)
    d_input = d_input.astype(jnp.bfloat16)
    factor = 1.0 / TOKENS ** 0.5
    gate_grad = jnp.dot(x_earlier.T, d_gate, preferred_element_type=jnp.float32)
    up_grad = jnp.dot(x_earlier.T, d_up, preferred_element_type=jnp.float32)
    taps_grad = jnp.stack([lax.optimization_barrier(jnp.sum(d_pre * padded[:, tap:tap + LEN], axis=(0, 1))) for tap in range(KW)], axis=0)
    bias_grad = lax.optimization_barrier(jnp.sum(d_pre, axis=(0, 1)))
    return (hidden, d_input, gate_sum + factor * gate_grad, up_sum + factor * up_grad, taps_sum + factor * taps_grad, bias_sum + factor * bias_grad)
```

```python
import jax
import jax.numpy as jnp
from jax import lax
from jax.sharding import PartitionSpec as P

PIECES = 2
F32 = jnp.float32
BF16 = jnp.bfloat16


def ring_order(n):
    return [i for i in range(0, n, 2)] + [i for i in range(n - 1 - n % 2, 0, -2)]


def place_of(me, n):
    half = me // 2
    return jnp.where(me % 2 == 0, half, n - 1 - half)


def index_of(place, n):
    return jnp.where(place < (n + 1) // 2, 2 * place, 2 * (n - 1 - place) + 1)


def after(value, *deps):
    return lax.optimization_barrier((value, *deps))[0]


def gather_rows(x, n_tp):
    if n_tp != 4:
        return lax.all_gather(x, "tp", axis=0, tiled=True)
    me = lax.axis_index("tp")
    rows = x.shape[0]
    core = [(i, i ^ 1) for i in range(4)]
    chip = [(i, i ^ 2) for i in range(4)]
    far = lax.ppermute(x, "tp", chip)
    near = lax.ppermute(x, "tp", core)
    both = lax.ppermute(far, "tp", core)
    out = jnp.zeros((rows * 4, x.shape[1]), x.dtype)
    for flip, piece in ((0, x), (1, near), (2, far), (3, both)):
        out = lax.dynamic_update_slice(out, piece, ((me ^ flip) * rows, 0))
    return out


def scatter_rows(x, n_tp):
    if n_tp != 4:
        return lax.psum_scatter(x, "tp", scatter_dimension=0, tiled=True)
    me = lax.axis_index("tp")
    rows = x.shape[0] // 4
    core = [(i, i ^ 1) for i in range(4)]
    chip = [(i, i ^ 2) for i in range(4)]

    def cut(flip):
        return lax.dynamic_slice(x, ((me ^ flip) * rows, 0), (rows, x.shape[1]))

    got_far = lax.ppermute(cut(3), "tp", core)
    got_near = lax.ppermute(cut(1), "tp", core)
    away = (cut(2).astype(F32) + got_far.astype(F32)).astype(BF16)
    other = lax.ppermute(away, "tp", chip)
    return (cut(0).astype(F32) + got_near.astype(F32) + other.astype(F32)).astype(BF16)


def conv_front(gate_lin, conv_taps, conv_bias):
    taps = conv_taps.shape[0]
    length = gate_lin.shape[0]
    padded = jnp.pad(gate_lin.astype(F32), ((taps - 1, 0), (0, 0)))
    pre = jnp.zeros(gate_lin.shape, F32) + conv_bias
    for tap in range(taps):
        pre = pre + padded[tap : tap + length] * conv_taps[tap]
    return (padded, pre)


def local(
    x_later,
    x_earlier,
    d_hidden,
    gate_weight,
    up_weight,
    conv_taps,
    conv_bias,
    gate_sum,
    up_sum,
    taps_sum,
    bias_sum,
):
    n = lax.axis_size("fs")
    n_tp = lax.axis_size("tp")
    depth, width = gate_weight.shape
    taps = conv_taps.shape[0]
    order = ring_order(n)
    me = lax.axis_index("fs")
    place = place_of(me, n)
    right = [(order[i], order[(i + 1) % n]) for i in range(n)]
    left = [(order[(i + 1) % n], order[i]) for i in range(n)]
    moves = (right, left)
    signs = (1, -1)
    cols = width // PIECES
    pieces = range(PIECES)
    ways = range(2)
    cut = [slice(c * cols, (c + 1) * cols) for c in pieces]

    def owner(which, steps):
        return index_of((place - signs[which] * steps + 2 * n) % n, n)

    rows_earlier = gather_rows(x_earlier, n_tp)
    rows_later = gather_rows(after(x_later, rows_earlier), n_tp)
    seq_rows = rows_earlier.shape[0]
    factor = 1.0 / (seq_rows * n) ** 0.5

    def turned(rows, which):
        return jnp.concatenate(
            [
                lax.dynamic_slice(rows, (0, owner(which, step) * depth), (seq_rows, depth))
                for step in range(n)
            ],
            axis=1,
        )

    def span(rows, first, last):
        return rows[:, first * depth : last * depth]

    blocks = [[[w[:, cut[c]]] for c in pieces] for w in (gate_weight, up_weight)]
    for step in range(n - 1):
        for c in pieces:
            for w in ways:
                blocks[w][c].append(lax.ppermute(blocks[w][c][step], "fs", moves[w]))
    half = n // 2
    earlier = [
        turned(after(rows_earlier, blocks[0][0][1], blocks[1][0][1]), w) for w in ways
    ]
    later = [turned(after(rows_later, blocks[0][0][3], blocks[1][0][3]), w) for w in ways]
    head = [[jnp.concatenate(blocks[w][c][:half], axis=0) for c in pieces] for w in ways]

    def dot(a, b):
        return jnp.dot(a, b, preferred_element_type=F32)

    acc = [[dot(span(earlier[w], 0, half), head[w][c]) for c in pieces] for w in ways]
    acc_later = [[dot(span(later[w], 0, half), head[w][c]) for c in pieces] for w in ways]
    marks = list(range(half, n - 1, 2)) + [n - 1, n]
    for first, last in zip(marks[:-2], marks[1:-1]):
        for c in pieces:
            for w in ways:
                body = jnp.concatenate(blocks[w][c][first:last], axis=0)
                acc[w][c] = acc[w][c] + dot(span(earlier[w], first, last), body)

    leading = (((0,), (0,)), ((), ()))
    d_lin = [[None for _ in pieces] for _ in ways]
    small = []

    def own_term(w, c, step):
        k = (step + 1) % n
        return lax.dot_general(
            span(earlier[w], k, k + 1), d_lin[w][c], leading, preferred_element_type=F32
        )

    run = [[None for _ in pieces] for _ in ways]
    begun = []
    for c in pieces:
        total = []
        for w in ways:
            block = after(blocks[w][c][n - 1], *begun) if begun else blocks[w][c][n - 1]
            total.append(acc[w][c] + dot(span(earlier[w], n - 1, n), block))
        gate_back, up_back = (t.astype(BF16) for t in total)
        padded, pre_back = conv_front(gate_back, conv_taps[:, cut[c]], conv_bias[cut[c]])
        act, pull = jax.vjp(jax.nn.gelu, pre_back)
        cot = d_hidden[:, cut[c]].astype(F32)
        d_lin[1][c] = (cot * act).astype(BF16)
        d_pre = pull(cot * up_back.astype(F32))[0]
        tail = jnp.pad(d_pre, ((0, taps - 1), (0, 0)))
        d_gate = jnp.zeros_like(d_pre)
        for tap in range(taps):
            begin = taps - 1 - tap
            d_gate = d_gate + tail[begin : begin + seq_rows] * conv_taps[tap, cut[c]]
        d_lin[0][c] = d_gate.astype(BF16)
        small.append(
            jnp.stack(
                [jnp.sum(d_pre * padded[tap : tap + seq_rows], axis=0) for tap in range(taps)]
                + [jnp.sum(d_pre, axis=0)],
                axis=0,
            )
        )
        for w in ways:
            run[w][c] = own_term(w, c, 0).astype(BF16)
            begun.append(run[w][c])

    stages = [begun]
    for step in range(1, n):
        nxt = [[None for _ in pieces] for _ in ways]
        for c in pieces:
            for w in ways:
                got = lax.ppermute(run[w][c], "fs", moves[w])
                total = got.astype(F32) + own_term(w, c, step)
                nxt[w][c] = total.astype(BF16) if step < n - 1 else total
        run = nxt
        stages.append([run[w][c] for w in ways for c in pieces])
    sums = [
        base + factor * jnp.concatenate(run[w], axis=1) for w, base in ((0, gate_sum), (1, up_sum))
    ]

    mine = jnp.concatenate(small, axis=1)
    if n & (n - 1) == 0:
        bit, stage = 1, 0
        while bit < n:
            mine = after(mine, *stages[min(stage, n - 2)])
            mine = mine + lax.ppermute(mine, "fs", [(i, i ^ bit) for i in range(n)])
            bit, stage = bit * 2, stage + 1
    else:
        mine = lax.psum(mine, "fs")

    transposed = (((1,), (1,)), ((), ()))
    rest = [[jnp.concatenate(blocks[w][c][half:], axis=0) for c in pieces] for w in ways]
    back = []
    for w in ways:
        spans = []
        for k, group in ((1, head), (2, rest)):
            term = None
            for c in pieces:
                cotangent = after(d_lin[w][c], *stages[k])
                part = lax.dot_general(
                    cotangent, group[w][c], transposed, preferred_element_type=F32
                )
                term = part if term is None else term + part
            spans.append(term)
        back.append(jnp.concatenate(spans, axis=1))
    columns = []
    for j in range(n):
        spot = order.index(j)
        slots = ((place - spot + n) % n, (spot - place + n) % n)
        columns.append(
            sum(
                lax.dynamic_slice(back[w], (0, slots[w] * depth), (seq_rows, depth))
                for w in ways
            ).astype(BF16)
        )
    d_input = scatter_rows(jnp.concatenate(columns, axis=1), n_tp)

    hidden = []
    for c in pieces:
        lin = []
        for w in ways:
            rows = after(span(later[w], half, n), *stages[min(3 + c, n - 2)])
            lin.append((acc_later[w][c] + dot(rows, rest[w][c])).astype(BF16))
        _, pre = conv_front(lin[0], conv_taps[:, cut[c]], conv_bias[cut[c]])
        hidden.append((jax.nn.gelu(pre) * lin[1].astype(F32)).astype(BF16))
    return (
        jnp.concatenate(hidden, axis=1),
        d_input,
        sums[0],
        sums[1],
        taps_sum + factor * mine[:taps],
        bias_sum + factor * mine[taps],
    )


def solution(mesh):
    placed = (
        P(("fs", "tp"), None),
        P(("fs", "tp"), None),
        P("fs", "tp"),
        P("fs", "tp"),
        P("fs", "tp"),
        P(None, "tp"),
        P("tp"),
        P("fs", "tp"),
        P("fs", "tp"),
        P(None, "tp"),
        P("tp"),
    )
    return jax.shard_map(
        local,
        mesh=mesh,
        in_specs=placed,
        out_specs=(
            P("fs", "tp"),
            P(("fs", "tp"), None),
            P("fs", "tp"),
            P("fs", "tp"),
            P(None, "tp"),
            P("tp"),
        ),
        check_vma=False,
    )
```

```python
import jax
import jax.numpy as jnp
from jax import lax
from jax.sharding import PartitionSpec as P


PIECES = 2
F32 = jnp.float32
BF16 = jnp.bfloat16


def ring_order(n):
    return [i for i in range(0, n, 2)] + [i for i in range(n - 1 - n % 2, 0, -2)]


def place_of(me, n):
    half = lax.shift_right_logical(me, 1)
    return jnp.where(lax.bitwise_and(me, 1) == 0, half, n - 1 - half)


def index_of(place, n):
    return jnp.where(place < (n + 1) // 2, 2 * place, 2 * (n - 1 - place) + 1)


def after(value, *deps):
    return lax.optimization_barrier((value, *deps))[0]


def gather_rows(x, n_tp):
    if n_tp != 4:
        return lax.all_gather(x, "tp", axis=0, tiled=True)
    me = lax.axis_index("tp")
    rows = x.shape[0]
    core = [(i, i ^ 1) for i in range(4)]
    chip = [(i, i ^ 2) for i in range(4)]
    far = lax.ppermute(x, "tp", chip)
    near = lax.ppermute(x, "tp", core)
    both = lax.ppermute(far, "tp", core)
    out = jnp.zeros((rows * 4, x.shape[1]), x.dtype)
    for flip, piece in ((0, x), (1, near), (2, far), (3, both)):
        out = lax.dynamic_update_slice(out, piece, ((me ^ flip) * rows, 0))
    return out


def scatter_rows(x, n_tp):
    if n_tp != 4:
        return lax.psum_scatter(x, "tp", scatter_dimension=0, tiled=True)
    me = lax.axis_index("tp")
    rows = x.shape[0] // 4
    core = [(i, i ^ 1) for i in range(4)]
    chip = [(i, i ^ 2) for i in range(4)]

    def cut(flip):
        return lax.dynamic_slice(x, ((me ^ flip) * rows, 0), (rows, x.shape[1]))

    got_far = lax.ppermute(cut(3), "tp", core)
    got_near = lax.ppermute(cut(1), "tp", core)
    away = (cut(2).astype(F32) + got_far.astype(F32)).astype(BF16)
    other = lax.ppermute(away, "tp", chip)
    return (cut(0).astype(F32) + got_near.astype(F32) + other.astype(F32)).astype(BF16)


def conv_front(gate_lin, conv_taps, conv_bias):
    taps = conv_taps.shape[0]
    length = gate_lin.shape[0]
    padded = jnp.pad(gate_lin.astype(F32), ((taps - 1, 0), (0, 0)))
    pre = jnp.zeros(gate_lin.shape, F32) + conv_bias
    for tap in range(taps):
        pre = pre + padded[tap : tap + length] * conv_taps[tap]
    return (padded, pre)


def local(
    x_later,
    x_earlier,
    d_hidden,
    gate_weight,
    up_weight,
    conv_taps,
    conv_bias,
    gate_sum,
    up_sum,
    taps_sum,
    bias_sum,
):
    n = lax.axis_size("fs")
    n_tp = lax.axis_size("tp")
    depth, width = gate_weight.shape
    taps = conv_taps.shape[0]
    order = ring_order(n)
    me = lax.axis_index("fs")
    place = place_of(me, n)
    right = [(order[i], order[(i + 1) % n]) for i in range(n)]
    left = [(order[(i + 1) % n], order[i]) for i in range(n)]
    moves = (right, left)
    signs = (1, -1)
    cols = width // PIECES
    pieces = range(PIECES)
    ways = range(2)
    cut = [slice(c * cols, (c + 1) * cols) for c in pieces]

    def owner(which, steps):
        return index_of(lax.rem(place - signs[which] * steps + 2 * n, n), n)

    rows_earlier = gather_rows(x_earlier, n_tp)
    rows_later = gather_rows(after(x_later, rows_earlier), n_tp)
    seq_rows = rows_earlier.shape[0]
    factor = 1.0 / (seq_rows * n) ** 0.5

    def turned(rows, which):
        return jnp.concatenate(
            [
                lax.dynamic_slice(rows, (0, owner(which, step) * depth), (seq_rows, depth))
                for step in range(n)
            ],
            axis=1,
        )

    def span(rows, first, last):
        return rows[:, first * depth : last * depth]

    blocks = [[[w[:, cut[c]]] for c in pieces] for w in (gate_weight, up_weight)]
    for step in range(n - 1):
        for c in pieces:
            for w in ways:
                blocks[w][c].append(lax.ppermute(blocks[w][c][step], "fs", moves[w]))
    half = n // 2
    earlier = [
        turned(after(rows_earlier, blocks[0][0][1], blocks[1][0][1]), w) for w in ways
    ]
    later = [turned(after(rows_later, blocks[0][0][3], blocks[1][0][3]), w) for w in ways]
    head = [[jnp.concatenate(blocks[w][c][:half], axis=0) for c in pieces] for w in ways]

    def dot(a, b):
        return jnp.dot(a, b, preferred_element_type=F32)

    acc = [[None for _ in pieces] for _ in ways]
    acc_later = [[None for _ in pieces] for _ in ways]
    for c in pieces:
        for w in ways:
            acc[w][c] = dot(span(earlier[w], 0, half), head[w][c])
            acc_later[w][c] = dot(span(later[w], 0, half), head[w][c])
    marks = list(range(half, n - 1, 2)) + [n - 1, n]
    for first, last in zip(marks[:-2], marks[1:-1]):
        for c in pieces:
            for w in ways:
                body = jnp.concatenate(blocks[w][c][first:last], axis=0)
                acc[w][c] = acc[w][c] + dot(span(earlier[w], first, last), body)

    leading = (((0,), (0,)), ((), ()))
    d_lin = [[None for _ in pieces] for _ in ways]
    small = []

    def own_terms(rows, cotangent):
        return lax.dot_general(rows, cotangent, leading, preferred_element_type=F32).astype(BF16)

    run = [[None for _ in pieces] for _ in ways]
    begun = []
    for c in pieces:
        total = []
        for w in ways:
            block = after(blocks[w][c][n - 1], *begun) if begun else blocks[w][c][n - 1]
            total.append(acc[w][c] + dot(span(earlier[w], n - 1, n), block))
        gate_back, up_back = (t.astype(BF16) for t in total)
        padded, pre_back = conv_front(gate_back, conv_taps[:, cut[c]], conv_bias[cut[c]])
        act, pull = jax.vjp(jax.nn.gelu, pre_back)
        cot = d_hidden[:, cut[c]].astype(F32)
        d_lin[1][c] = (cot * act).astype(BF16)
        d_pre = pull(cot * up_back.astype(F32))[0]
        tail = jnp.pad(d_pre, ((0, taps - 1), (0, 0)))
        d_gate = jnp.zeros_like(d_pre)
        for tap in range(taps):
            begin = taps - 1 - tap
            d_gate = d_gate + tail[begin : begin + seq_rows] * conv_taps[tap, cut[c]]
        d_lin[0][c] = d_gate.astype(BF16)
        small.append(
            jnp.stack(
                [jnp.sum(d_pre * padded[tap : tap + seq_rows], axis=0) for tap in range(taps)]
                + [jnp.sum(d_pre, axis=0)],
                axis=0,
            )
        )
        for w in ways:
            run[w][c] = own_terms(span(earlier[w], 1, 2), d_lin[w][c])
            begun.append(run[w][c])

    stages = [begun]
    tail_rows = [jnp.concatenate([span(earlier[w], 2, n), span(earlier[w], 0, 1)], 1) for w in ways]
    own = [
        [own_terms(tail_rows[w], after(d_lin[w][c], *begun)) for c in pieces] for w in ways
    ]
    for step in range(1, n):
        nxt = [[None for _ in pieces] for _ in ways]
        for c in pieces:
            for w in ways:
                got = lax.ppermute(run[w][c], "fs", moves[w])
                mine = own[w][c][(step - 1) * depth : step * depth]
                total = got.astype(F32) + mine.astype(F32)
                nxt[w][c] = total.astype(BF16) if step < n - 1 else total
        run = nxt
        stages.append([run[w][c] for w in ways for c in pieces])
    sums = [
        base + factor * jnp.concatenate(run[w], axis=1) for w, base in ((0, gate_sum), (1, up_sum))
    ]

    mine = jnp.concatenate(small, axis=1)
    if n & (n - 1) == 0:
        bit, stage = 1, 1
        mine = after(mine, *stages[1])
        while bit < n:
            got = lax.ppermute(mine, "fs", [(i, i ^ bit) for i in range(n)])
            mine = mine + after(got, *stages[min(stage + 1, n - 2)])
            bit, stage = bit * 2, stage + 1
    else:
        mine = lax.psum(mine, "fs")

    transposed = (((1,), (1,)), ((), ()))
    rest = [[jnp.concatenate(blocks[w][c][half:], axis=0) for c in pieces] for w in ways]
    back = []
    for w in ways:
        spans = []
        for k, group in ((1, head), (2, rest)):
            term = None
            for c in pieces:
                cotangent = after(d_lin[w][c], *stages[k])
                part = lax.dot_general(
                    cotangent, group[w][c], transposed, preferred_element_type=F32
                )
                term = part if term is None else term + part
            spans.append(term)
        back.append(jnp.concatenate(spans, axis=1))
    columns = []
    for j in range(n):
        spot = order.index(j)
        slots = (lax.rem(place - spot + n, n), lax.rem(spot - place + n, n))
        columns.append(
            sum(
                lax.dynamic_slice(back[w], (0, slots[w] * depth), (seq_rows, depth))
                for w in ways
            ).astype(BF16)
        )
    d_input = scatter_rows(jnp.concatenate(columns, axis=1), n_tp)

    hidden = []
    for c in pieces:
        lin = []
        for w in ways:
            rows = after(span(later[w], half, n), *stages[min(3 + c, n - 2)])
            lin.append((acc_later[w][c] + dot(rows, rest[w][c])).astype(BF16))
        _, pre = conv_front(lin[0], conv_taps[:, cut[c]], conv_bias[cut[c]])
        hidden.append((jax.nn.gelu(pre) * lin[1].astype(F32)).astype(BF16))
    return (
        jnp.concatenate(hidden, axis=1),
        d_input,
        sums[0],
        sums[1],
        taps_sum + factor * mine[:taps],
        bias_sum + factor * mine[taps],
    )


def solution(mesh):
    placed = (
        P(("fs", "tp"), None),
        P(("fs", "tp"), None),
        P("fs", "tp"),
        P("fs", "tp"),
        P("fs", "tp"),
        P(None, "tp"),
        P("tp"),
        P("fs", "tp"),
        P("fs", "tp"),
        P(None, "tp"),
        P("tp"),
    )
    return jax.shard_map(
        local,
        mesh=mesh,
        in_specs=placed,
        out_specs=(
            P("fs", "tp"),
            P(("fs", "tp"), None),
            P("fs", "tp"),
            P("fs", "tp"),
            P(None, "tp"),
            P("tp"),
        ),
        check_vma=False,
    )
```
